32 devices in a mesh: fs: 16 (over z, y, x), tp: 2 (over core).
Axes of the slice: x: 2, y: 2, z: 4, core: 2. Of those that a mesh axis runs over, the one named last changes fastest.
Arguments:
- saved_inputs: bfloat16 [2048, 4096], P('fs', 'tp'), may hold values from -6 to 6
- value_cotangent: bfloat16 [2048, 2048], P('fs'), may hold values from -0.1875 to 0.1875
- glu_output: bfloat16 [2048, 2048], P('fs', 'tp'), may hold values from -6 to 6
- conv_cotangent: bfloat16 [2048, 2048], P('fs', 'tp'), may hold values from -0.125 to 0.125
- factor: bfloat16 [4096, 256], P('tp'), may hold values from -0.09375 to 0.09375
- value_weight: float32 [2048, 4096], P('fs', 'tp'), may hold values from -3 to 3
- first_moment: float32 [2048, 256], P('fs', 'tp'), may hold values from -6 to 6
- second_moment: float32 [2048, 256], P('fs', 'tp'), may hold values from 0.25 to 4
- kernel: float32 [31, 2048], P(None, 'tp'), may hold values from -1 to 1
- kernel_first: float32 [31, 2048], P(None, 'tp'), may hold values from -6 to 6
- kernel_second: float32 [31, 2048], P(None, 'tp'), may hold values from 0.25 to 4
Outputs:
- new_value: float32 [2048, 4096], P('fs', 'tp')
- value_copy: bfloat16 [2048, 4096], P('fs', 'tp')
- value_step: float32 [2048, 4096], P('fs', 'tp')
- new_first: float32 [2048, 256], P('fs', 'tp')
- new_second: float32 [2048, 256], P('fs', 'tp')
- new_kernel: float32 [31, 2048], P(None, 'tp')
- new_kernel_first: float32 [31, 2048], P(None, 'tp')
- new_kernel_second: float32 [31, 2048], P(None, 'tp')
The draws below stay inside these ranges and needn't reach their ends.
All inputs are finite; a program needn't handle non-finite values.
Results may differ from the reference program's by a relative error of at most 0.0055.
Values may be sent and summed in bfloat16 or wider, within the bound.
A program may use at most 64 MiB of HBM per device.

```python
import math
import jax
import jax.numpy as jnp
from jax import lax

WIDTH = 4096
CHANNELS = 2048
TAPS = 31
RANK = 256
TOKENS = 2048


def spiked(entries, own_key, source, target, parts, factor):
    def block_of(axis_at):
        return (jnp.arange(entries.shape[axis_at]) // (entries.shape[axis_at] // parts)).reshape((-1,) + (1,) * (entries.ndim - 1 - axis_at))

    first = jax.random.permutation(own_key, parts)[block_of(target)]
    second = (block_of(target) + parts // 2) % parts
    return jnp.where((block_of(source) == first) | (block_of(source) == second), factor * entries, entries)


def shard_levels(rng, dims, split, least, top_value):
    factor_of, own = 1.0, jax.random.fold_in(rng, 6)
    for position, parts in split:
        heights = jnp.exp(jax.random.uniform(jax.random.fold_in(own, position), (parts,), jnp.float32, least / len(split), top_value / len(split)))
        factor_of = factor_of * jnp.repeat(heights, dims[position] // parts).reshape([-1 if axis == position else 1 for axis in range(len(dims))])
    return factor_of


def noise(stream_key, extent, width, limit, shards=(), kind=jnp.bfloat16):
    drawn = width * jax.random.normal(stream_key, extent, jnp.float32)
    if shards:
        drawn = drawn * shard_levels(stream_key, extent, shards, -0.22, 0.18)
    return jnp.clip(drawn, -limit, limit).astype(kind)


def gaussian_with(rng, extent, width, bound, cuts, heavy, dtype=jnp.bfloat16):
    values = width * jax.random.normal(rng, extent, jnp.float32)
    if cuts:
        values = values * shard_levels(rng, extent, cuts, -0.22, 0.18)
    return jnp.clip(spiked(values, jax.random.fold_in(rng, 3), *heavy), -bound, bound).astype(dtype)


def setup_inputs(seed: int = 0) -> dict:
    arg_keys = jax.random.split(jax.random.key(seed), 12)
    saved_inputs = noise(arg_keys[0], (TOKENS, WIDTH), 1.0, 6.0, ((0, 16), (1, 2)))
    value_cotangent = gaussian_with(arg_keys[1], (TOKENS, CHANNELS), (TOKENS ** -0.5), 0.1875, ((0, 16),), (0, 1, 16, 2.0))
    glu_output = noise(arg_keys[2], (TOKENS, CHANNELS), 1.0, 6.0, ((0, 16), (1, 2)))
    conv_cotangent = noise(arg_keys[3], (TOKENS, CHANNELS), (TOKENS ** -0.5), 0.125, ((0, 16), (1, 2)))
    factor = noise(arg_keys[4], (WIDTH, RANK), WIDTH ** -0.5, 0.09375, ((0, 2),))
    value_weight = noise(arg_keys[5], (CHANNELS, WIDTH), 0.5, 3.0, ((0, 16), (1, 2)), jnp.float32)
    first_moment = noise(arg_keys[6], (CHANNELS, RANK), 1.0, 6.0, ((0, 16), (1, 2)), jnp.float32)
    second_moment = jnp.clip(jnp.exp(math.log(4.0) - 2.7725887 * jax.random.uniform(arg_keys[7], (CHANNELS, RANK), jnp.float32) ** shard_levels(arg_keys[7], (CHANNELS, RANK), ((0, 16), (1, 2)), -0.2, 0.2)), 0.25, 4.0)
    kernel = noise(arg_keys[8], (TAPS, CHANNELS), TAPS ** -0.5, 1.0, ((1, 2),), jnp.float32)
    kernel_first = noise(arg_keys[9], (TAPS, CHANNELS), 1.0, 6.0, ((1, 2),), jnp.float32)
    kernel_second = jnp.clip(jnp.exp(math.log(4.0) - 2.7725887 * jax.random.uniform(arg_keys[10], (TAPS, CHANNELS), jnp.float32) ** shard_levels(arg_keys[10], (TAPS, CHANNELS), ((1, 2),), -0.2, 0.2)), 0.25, 4.0)
    return {"saved_inputs": saved_inputs, "value_cotangent": value_cotangent, "glu_output": glu_output, "conv_cotangent": conv_cotangent, "factor": factor, "value_weight": value_weight, "first_moment": first_moment, "second_moment": second_moment, "kernel": kernel, "kernel_first": kernel_first, "kernel_second": kernel_second}


def reference(saved_inputs, value_cotangent, glu_output, conv_cotangent, factor, value_weight, first_moment, second_moment, kernel, kernel_first, kernel_second):
    highest = lax.Precision.HIGHEST
    gradient = jnp.dot(value_cotangent.astype(jnp.float32).T, saved_inputs.astype(jnp.float32), precision=highest, preferred_element_type=jnp.float32)
    factor_f = factor.astype(jnp.float32)
    projected = jnp.dot(gradient, factor_f, precision=highest)
    new_first = 0.8 * first_moment + 0.2 * projected
    new_second = 0.9 * second_moment + 0.1 * projected * projected
    direction = new_first / jnp.sqrt(new_second)
    back_proj = jnp.dot(direction, factor_f.T, precision=highest)
    row_mean = lax.optimization_barrier(jnp.mean(back_proj * back_proj, axis=1, keepdims=True))
    value_step = back_proj / jnp.sqrt(row_mean + 0.01)
    new_value = value_weight - 0.05 * value_step
    value_copy = new_value.astype(jnp.bfloat16)
    padded = jnp.pad(glu_output.astype(jnp.float32), ((TAPS - 1, 0), (0, 0)))
    cotangent_f = conv_cotangent.astype(jnp.float32)
    pieces = []
    for offset in range(TAPS):
        begin = TAPS - 1 - offset
        pieces.append(lax.optimization_barrier(jnp.sum(padded[begin:begin + TOKENS] * cotangent_f, axis=0)))
    kernel_grad = jnp.stack(pieces, axis=0)
    new_kernel_first = 0.8 * kernel_first + 0.2 * kernel_grad
    new_kernel_second = 0.9 * kernel_second + 0.1 * kernel_grad * kernel_grad
    new_kernel = kernel - 0.05 * new_kernel_first / jnp.sqrt(new_kernel_second)
    return (new_value, value_copy, value_step, new_first, new_second, new_kernel, new_kernel_first, new_kernel_second)
```

```python
import functools

import jax
import jax.numpy as jnp
from jax import lax
from jax.experimental import pallas as pl
from jax.experimental.pallas import tpu as pltpu
from jax.sharding import PartitionSpec as P

MESH = pl.DeviceIdType.MESH
LANES = 128
f32 = jnp.float32
bf16 = jnp.bfloat16


def remote(src, dst, send, recv, axis, peer):
    return pltpu.make_async_remote_copy(
        src_ref=src,
        dst_ref=dst,
        send_sem=send,
        recv_sem=recv,
        device_id={axis: peer},
        device_id_type=MESH,
    )


def reduce_kernel(
    n,
    m,
    x_ref,
    v_ref,
    g_ref,
    c_ref,
    f_ref,
    m1_ref,
    m2_ref,
    proj_ref,
    kg_ref,
    dn_ref,
    low_out,
    low_in,
    gram,
    part,
    recv,
    halo,
    ext,
    cot,
    stage,
    tap_out,
    tap_in,
    tap_all,
    dirs,
    low_s,
    low_r,
    gram_s,
    gram_r,
    bulk_s,
    bulk_r,
    halo_s,
    halo_r,
    tap_s,
    tap_r,
    all_s,
    all_r,
    dir_s,
    dir_r,
):
    me = lax.axis_index("fs")
    my = lax.axis_index("tp")
    tokens = x_ref.shape[0]
    width = f_ref.shape[0] * m
    rows, cols = m1_ref.shape
    reach = halo.shape[0]
    groups = ext.shape[0]
    taps = kg_ref.shape[0]
    padded = stage.shape[0] // groups

    def peers(count, own, fn):
        def step(off, carry):
            fn(off, lax.rem(own + off, count))
            return carry

        lax.fori_loop(1, count, step, 0)

    barrier = pltpu.get_barrier_semaphore()
    peers(n, me, lambda off, p: pl.semaphore_signal(barrier, inc=1, device_id={"fs": p}, device_id_type=MESH))
    peers(m, my, lambda off, p: pl.semaphore_signal(barrier, inc=1, device_id={"tp": p}, device_id_type=MESH))

    low = jnp.dot(x_ref[...], f_ref[...], preferred_element_type=f32).astype(bf16)
    for j in range(m):
        low_out[j] = low[:, j * cols : (j + 1) * cols]

    pl.semaphore_wait(barrier, n - 1 + m - 1)

    def low_copy(off, p):
        return remote(low_out.at[p], low_in.at[my], low_s.at[off], low_r.at[off], "tp", p)

    peers(m, my, lambda off, p: low_copy(off, p).start())
    low_in[my] = low_out[my]
    after = lax.rem(me + 1, n)
    halo_copy = remote(
        g_ref.at[pl.ds(tokens - reach, reach)], halo, halo_s, halo_r, "fs", after
    )
    halo_copy.start()

    peers(m, my, lambda off, p: low_copy(off, p).wait())
    reduced = low_in[0].astype(f32)
    for j in range(1, m):
        reduced = reduced + low_in[j].astype(f32)
    reduced = reduced.astype(bf16)

    part[...] = (
        lax.dot_general(v_ref[...], reduced, (((0,), (0,)), ((), ())), preferred_element_type=f32)
        .astype(bf16)
        .reshape(n, rows, cols)
    )

    def bulk_copy(off, p):
        return remote(part.at[p], recv.at[me], bulk_s.at[off], bulk_r.at[off], "fs", p)

    peers(n, me, lambda off, p: bulk_copy(off, p).start())
    recv[me] = part[me]

    halo_copy.wait()
    halo_f = jnp.where(me > 0, halo[...].astype(f32), 0.0)
    for g in range(groups):
        lanes = slice(g * LANES, (g + 1) * LANES)
        ext[g, :reach] = halo_f[:, lanes]
        ext[g, reach:] = g_ref[:, lanes].astype(f32)
        cot[g] = c_ref[:, lanes].astype(f32)

    def group_step(g, carry):
        right = cot[g]
        sums = []
        for k in range(taps):
            product = ext[g, pl.ds(reach - k, tokens), :] * right
            sums.append(jnp.sum(product, axis=0, keepdims=True))
        sums.append(jnp.zeros((padded - taps, LANES), f32))
        stage[pl.ds(pl.multiple_of(g * padded, padded), padded), :] = jnp.concatenate(sums, axis=0)
        return carry

    lax.fori_loop(0, groups, group_step, 0)
    tap_out[...] = stage[...].reshape(tap_out.shape).astype(bf16)

    def tap_copy(off, p):
        return remote(tap_out.at[p], tap_in.at[me], tap_s.at[off], tap_r.at[off], "fs", p)

    peers(n, me, lambda off, p: tap_copy(off, p).start())
    tap_in[me] = tap_out[me]

    gram[my] = lax.dot_general(
        f_ref[...], f_ref[...], (((0,), (0,)), ((), ())), preferred_element_type=f32
    )

    def gram_copy(off, p):
        return remote(gram.at[my], gram.at[my], gram_s.at[off], gram_r.at[off], "tp", p)

    peers(m, my, lambda off, p: gram_copy(off, p).start())

    peers(n, me, lambda off, p: bulk_copy(off, p).wait())
    projected = recv[0].astype(f32)
    for j in range(1, n):
        projected = projected + recv[j].astype(f32)
    proj_ref[...] = projected
    first = 0.8 * m1_ref[...] + 0.2 * projected
    second = 0.9 * m2_ref[...] + 0.1 * projected * projected
    dirs[my] = first / jnp.sqrt(second)

    def dir_copy(off, p):
        return remote(dirs.at[my], dirs.at[my], dir_s.at[off], dir_r.at[off], "tp", p)

    peers(m, my, lambda off, p: dir_copy(off, p).start())

    peers(n, me, lambda off, p: tap_copy(off, p).wait())
    tap_all[me] = jnp.sum(tap_in[...].astype(f32), axis=0).astype(bf16)

    def all_copy(off, p):
        return remote(tap_all.at[me], tap_all.at[me], all_s.at[off], all_r.at[off], "fs", p)

    peers(n, me, lambda off, p: all_copy(off, p).start())

    peers(m, my, lambda off, p: gram_copy(off, p).wait())
    total = gram[0]
    for j in range(1, m):
        total = total + gram[j]
    peers(m, my, lambda off, p: dir_copy(off, p).wait())
    direction = jnp.concatenate([dirs[j] for j in range(m)], axis=1)
    turned = jnp.dot(direction, total, precision=lax.Precision.HIGHEST, preferred_element_type=f32)
    mean = jnp.sum(turned * direction, axis=1, keepdims=True) / width
    dn_ref[...] = direction / jnp.sqrt(mean + 0.01)

    peers(n, me, lambda off, p: all_copy(off, p).wait())
    stage[...] = tap_all[...].astype(f32).reshape(stage.shape)
    for g in range(groups):
        kg_ref[:, g * LANES : (g + 1) * LANES] = stage[g * padded : g * padded + taps, :]


def update_kernel(
    dn_ref,
    f_ref,
    w_ref,
    proj_ref,
    m1_ref,
    m2_ref,
    kg_ref,
    k_ref,
    k1_ref,
    k2_ref,
    value_ref,
    copy_ref,
    step_ref,
    n1_ref,
    n2_ref,
    nk_ref,
    nk1_ref,
    nk2_ref,
):
    dn = dn_ref[...]
    upper = dn.astype(bf16)
    lower = (dn - upper.astype(f32)).astype(bf16)
    factor = f_ref[...]
    dims = (((1,), (1,)), ((), ()))
    step = lax.dot_general(upper, factor, dims, preferred_element_type=f32)
    step = step + lax.dot_general(lower, factor, dims, preferred_element_type=f32)
    step_ref[...] = step
    value = w_ref[...] - 0.05 * step
    value_ref[...] = value
    copy_ref[...] = value.astype(bf16)

    @pl.when(pl.program_id(0) == 0)
    def _():
        projected = proj_ref[...]
        n1_ref[...] = 0.8 * m1_ref[...] + 0.2 * projected
        n2_ref[...] = 0.9 * m2_ref[...] + 0.1 * projected * projected
        grad = kg_ref[...]
        first = 0.8 * k1_ref[...] + 0.2 * grad
        second = 0.9 * k2_ref[...] + 0.1 * grad * grad
        nk1_ref[...] = first
        nk2_ref[...] = second
        nk_ref[...] = k_ref[...] - 0.05 * first / jnp.sqrt(second)


def body(n, m, x, v, g, c, f, w, m1, m2, k, k1, k2):
    tokens = x.shape[0]
    features, rank = f.shape
    rows, cols = m1.shape
    taps, channels = k.shape
    groups = channels // LANES
    reach = -(-(taps - 1) // 16) * 16
    padded = -(-taps // 8) * 8
    chunk = groups * padded // n
    vmem = pl.BlockSpec(memory_space=pltpu.VMEM)
    dma = pltpu.SemaphoreType.DMA
    proj, kg, dn = pl.pallas_call(
        functools.partial(reduce_kernel, n, m),
        out_shape=(
            jax.ShapeDtypeStruct((rows, cols), f32),
            jax.ShapeDtypeStruct((taps, channels), f32),
            jax.ShapeDtypeStruct((rows, rank), f32),
        ),
        in_specs=[vmem] * 7,
        out_specs=(vmem,) * 3,
        scratch_shapes=[
            pltpu.VMEM((m, tokens, cols), bf16),
            pltpu.VMEM((m, tokens, cols), bf16),
            pltpu.VMEM((m, rank, rank), f32),
            pltpu.VMEM((n, rows, cols), bf16),
            pltpu.VMEM((n, rows, cols), bf16),
            pltpu.VMEM((reach, channels), bf16),
            pltpu.VMEM((groups, reach + tokens, LANES), f32),
            pltpu.VMEM((groups, tokens, LANES), f32),
            pltpu.VMEM((groups * padded, LANES), f32),
            pltpu.VMEM((n, chunk, LANES), bf16),
            pltpu.VMEM((n, chunk, LANES), bf16),
            pltpu.VMEM((n, chunk, LANES), bf16),
            pltpu.VMEM((m, rows, cols), f32),
            dma((m,)),
            dma((m,)),
            dma((m,)),
            dma((m,)),
            dma((n,)),
            dma((n,)),
            dma,
            dma,
            dma((n,)),
            dma((n,)),
            dma((n,)),
            dma((n,)),
            dma((m,)),
            dma((m,)),
        ],
        compiler_params=pltpu.CompilerParams(collective_id=0, has_side_effects=True),
        name="reduce",
    )(x, v, g, c, f, m1, m2)

    steps = 4 if features % (4 * LANES) == 0 else 1
    block = features // steps
    whole = lambda a: pl.BlockSpec(a.shape, lambda i: (0, 0))
    wide = pl.BlockSpec((rows, block), lambda i: (0, i))
    return pl.pallas_call(
        update_kernel,
        grid=(steps,),
        out_shape=(
            jax.ShapeDtypeStruct(w.shape, f32),
            jax.ShapeDtypeStruct(w.shape, bf16),
            jax.ShapeDtypeStruct(w.shape, f32),
            jax.ShapeDtypeStruct(m1.shape, f32),
            jax.ShapeDtypeStruct(m1.shape, f32),
            jax.ShapeDtypeStruct(k.shape, f32),
            jax.ShapeDtypeStruct(k.shape, f32),
            jax.ShapeDtypeStruct(k.shape, f32),
        ),
        in_specs=[
            whole(dn),
            pl.BlockSpec((block, rank), lambda i: (i, 0)),
            wide,
            whole(proj),
            whole(m1),
            whole(m2),
            whole(kg),
            whole(k),
            whole(k1),
            whole(k2),
        ],
        out_specs=(wide, wide, wide, whole(m1), whole(m1), whole(k), whole(k), whole(k)),
        compiler_params=pltpu.CompilerParams(dimension_semantics=("arbitrary",)),
        name="update",
    )(dn, f, w, proj, m1, m2, kg, k, k1, k2)


def solution(mesh):
    both, rows, cols = P("fs", "tp"), P("fs", None), P(None, "tp")
    return jax.shard_map(
        functools.partial(body, mesh.shape["fs"], mesh.shape["tp"]),
        mesh=mesh,
        in_specs=(both, rows, both, both, P("tp", None), both, both, both, cols, cols, cols),
        out_specs=(both, both, both, both, both, cols, cols, cols),
        check_vma=False,
    )
```

```python
import functools

import jax
import jax.numpy as jnp
from jax import lax
from jax.experimental import pallas as pl
from jax.experimental.pallas import tpu as pltpu
from jax.sharding import PartitionSpec as P

MESH = pl.DeviceIdType.MESH
LANES = 128
f32 = jnp.float32
bf16 = jnp.bfloat16


def remote(src, dst, send, recv, axis, peer):
    return pltpu.make_async_remote_copy(
        src_ref=src,
        dst_ref=dst,
        send_sem=send,
        recv_sem=recv,
        device_id={axis: peer},
        device_id_type=MESH,
    )


def reduce_kernel(
    n,
    m,
    x_hbm,
    v_hbm,
    g_hbm,
    c_hbm,
    f_hbm,
    m1_hbm,
    m2_hbm,
    proj_ref,
    kg_ref,
    dn_ref,
    x_ref,
    v_ref,
    g_ref,
    c_ref,
    f_ref,
    m1_ref,
    m2_ref,
    load_s,
    low_out,
    low_in,
    gram,
    part,
    recv,
    halo,
    ext,
    cot,
    stage,
    tap_out,
    tap_in,
    tap_all,
    dirs,
    low_s,
    low_r,
    gram_s,
    gram_r,
    bulk_s,
    bulk_r,
    halo_s,
    halo_r,
    tap_s,
    tap_r,
    all_s,
    all_r,
    dir_s,
    dir_r,
):
    me = lax.axis_index("fs")
    my = lax.axis_index("tp")
    tokens = x_ref.shape[0]
    width = f_ref.shape[0] * m
    rows, cols = m1_ref.shape
    reach = halo.shape[0]
    groups = ext.shape[0]
    taps = kg_ref.shape[0]
    padded = stage.shape[0] // groups

    def peers(count, own, fn):
        def step(off, carry):
            fn(off, lax.rem(own + off, count))
            return carry

        lax.fori_loop(1, count, step, 0)

    barrier = pltpu.get_barrier_semaphore()
    peers(n, me, lambda off, p: pl.semaphore_signal(barrier, inc=1, device_id={"fs": p}, device_id_type=MESH))
    peers(m, my, lambda off, p: pl.semaphore_signal(barrier, inc=1, device_id={"tp": p}, device_id_type=MESH))

    pairs = [(x_hbm, x_ref), (f_hbm, f_ref), (g_hbm, g_ref), (c_hbm, c_ref)]
    pairs += [(v_hbm, v_ref), (m1_hbm, m1_ref), (m2_hbm, m2_ref)]
    loads = [pltpu.make_async_copy(a, b, load_s.at[i]) for i, (a, b) in enumerate(pairs)]
    for load in loads:
        load.start()
    loads[0].wait()
    loads[1].wait()

    low = jnp.dot(x_ref[...], f_ref[...], preferred_element_type=f32).astype(bf16)
    for j in range(m):
        low_out[j] = low[:, j * cols : (j + 1) * cols]

    loads[2].wait()
    loads[3].wait()
    for g in range(groups):
        lanes = slice(g * LANES, (g + 1) * LANES)
        ext[g, :reach] = jnp.zeros((reach, LANES), f32)
        ext[g, reach:] = g_ref[:, lanes].astype(f32)
        cot[g] = c_ref[:, lanes].astype(f32)

    def group_step(count, add):
        def step(g, carry):
            right = cot[g, :count, :]
            sums = []
            for k in range(taps):
                product = ext[g, pl.ds(reach - k, count), :] * right
                sums.append(jnp.sum(product, axis=0, keepdims=True))
            sums.append(jnp.zeros((padded - taps, LANES), f32))
            at = pl.ds(pl.multiple_of(g * padded, padded), padded)
            block = jnp.concatenate(sums, axis=0)
            stage[at, :] = stage[at, :] + block if add else block
            return carry

        lax.fori_loop(0, groups, step, 0)

    group_step(tokens, False)

    pl.semaphore_wait(barrier, n - 1 + m - 1)

    def low_copy(off, p):
        return remote(low_out.at[p], low_in.at[my], low_s.at[off], low_r.at[off], "tp", p)

    peers(m, my, lambda off, p: low_copy(off, p).start())
    low_in[my] = low_out[my]
    after = lax.rem(me + 1, n)
    halo_copy = remote(
        g_ref.at[pl.ds(tokens - reach, reach)], halo, halo_s, halo_r, "fs", after
    )
    halo_copy.start()

    halo_copy.wait()
    halo_f = jnp.where(me > 0, halo[...].astype(f32), 0.0)
    for g in range(groups):
        ext[g, :reach] = halo_f[:, g * LANES : (g + 1) * LANES]
        ext[g, reach:] = jnp.zeros((tokens, LANES), f32)
    group_step(reach, True)
    tap_out[...] = stage[...].reshape(tap_out.shape).astype(bf16)

    def tap_copy(off, p):
        return remote(tap_out.at[p], tap_in.at[me], tap_s.at[off], tap_r.at[off], "fs", p)

    peers(n, me, lambda off, p: tap_copy(off, p).start())
    tap_in[me] = tap_out[me]
    loads[4].wait()

    peers(m, my, lambda off, p: low_copy(off, p).wait())
    reduced = low_in[0].astype(f32)
    for j in range(1, m):
        reduced = reduced + low_in[j].astype(f32)
    reduced = reduced.astype(bf16)

    part[...] = (
        lax.dot_general(v_ref[...], reduced, (((0,), (0,)), ((), ())), preferred_element_type=f32)
        .astype(bf16)
        .reshape(n, rows, cols)
    )

    def bulk_copy(off, p):
        return remote(part.at[p], recv.at[me], bulk_s.at[off], bulk_r.at[off], "fs", p)

    peers(n, me, lambda off, p: bulk_copy(off, p).start())
    recv[me] = part[me]

    gram[my] = lax.dot_general(
        f_ref[...], f_ref[...], (((0,), (0,)), ((), ())), preferred_element_type=f32
    )

    def gram_copy(off, p):
        return remote(gram.at[my], gram.at[my], gram_s.at[off], gram_r.at[off], "tp", p)

    peers(m, my, lambda off, p: gram_copy(off, p).start())

    peers(n, me, lambda off, p: tap_copy(off, p).wait())
    tap_all[me] = jnp.sum(tap_in[...].astype(f32), axis=0).astype(bf16)

    def all_copy(off, p):
        return remote(tap_all.at[me], tap_all.at[me], all_s.at[off], all_r.at[off], "fs", p)

    peers(n, me, lambda off, p: all_copy(off, p).start())

    loads[5].wait()
    loads[6].wait()
    peers(n, me, lambda off, p: bulk_copy(off, p).wait())
    projected = recv[0].astype(f32)
    for j in range(1, n):
        projected = projected + recv[j].astype(f32)
    proj_ref[...] = projected
    first = 0.8 * m1_ref[...] + 0.2 * projected
    second = 0.9 * m2_ref[...] + 0.1 * projected * projected
    dirs[my] = first / jnp.sqrt(second)

    def dir_copy(off, p):
        return remote(dirs.at[my], dirs.at[my], dir_s.at[off], dir_r.at[off], "tp", p)

    peers(m, my, lambda off, p: dir_copy(off, p).start())

    peers(m, my, lambda off, p: gram_copy(off, p).wait())
    total = gram[0]
    for j in range(1, m):
        total = total + gram[j]
    peers(m, my, lambda off, p: dir_copy(off, p).wait())
    direction = jnp.concatenate([dirs[j] for j in range(m)], axis=1)
    turned = jnp.dot(direction, total, precision=lax.Precision.HIGHEST, preferred_element_type=f32)
    mean = jnp.sum(turned * direction, axis=1, keepdims=True) / width
    dn_ref[...] = (direction / jnp.sqrt(mean + 0.01)).astype(bf16)

    peers(n, me, lambda off, p: all_copy(off, p).wait())
    stage[...] = tap_all[...].astype(f32).reshape(stage.shape)
    for g in range(groups):
        kg_ref[:, g * LANES : (g + 1) * LANES] = stage[g * padded : g * padded + taps, :]


def update_kernel(
    dn_ref,
    f_ref,
    w_ref,
    proj_ref,
    m1_ref,
    m2_ref,
    kg_ref,
    k_ref,
    k1_ref,
    k2_ref,
    value_ref,
    copy_ref,
    step_ref,
    n1_ref,
    n2_ref,
    nk_ref,
    nk1_ref,
    nk2_ref,
):
    dims = (((1,), (1,)), ((), ()))
    step = lax.dot_general(dn_ref[...], f_ref[...], dims, preferred_element_type=f32)
    step_ref[...] = step
    value = w_ref[...] - 0.05 * step
    value_ref[...] = value
    copy_ref[...] = value.astype(bf16)

    @pl.when(pl.program_id(0) == 0)
    def _():
        projected = proj_ref[...]
        n1_ref[...] = 0.8 * m1_ref[...] + 0.2 * projected
        n2_ref[...] = 0.9 * m2_ref[...] + 0.1 * projected * projected
        grad = kg_ref[...]
        first = 0.8 * k1_ref[...] + 0.2 * grad
        second = 0.9 * k2_ref[...] + 0.1 * grad * grad
        nk1_ref[...] = first
        nk2_ref[...] = second
        nk_ref[...] = k_ref[...] - 0.05 * first / jnp.sqrt(second)


def body(n, m, x, v, g, c, f, w, m1, m2, k, k1, k2):
    tokens = x.shape[0]
    features, rank = f.shape
    rows, cols = m1.shape
    taps, channels = k.shape
    groups = channels // LANES
    reach = -(-(taps - 1) // 16) * 16
    padded = -(-taps // 8) * 8
    chunk = groups * padded // n
    vmem = pl.BlockSpec(memory_space=pltpu.VMEM)
    dma = pltpu.SemaphoreType.DMA
    proj, kg, dn = pl.pallas_call(
        functools.partial(reduce_kernel, n, m),
        out_shape=(
            jax.ShapeDtypeStruct((rows, cols), f32),
            jax.ShapeDtypeStruct((taps, channels), f32),
            jax.ShapeDtypeStruct((rows, rank), bf16),
        ),
        in_specs=[pl.BlockSpec(memory_space=pl.ANY)] * 7,
        out_specs=(vmem,) * 3,
        scratch_shapes=[
            *(pltpu.VMEM(a.shape, a.dtype) for a in (x, v, g, c, f, m1, m2)),
            dma((7,)),
            pltpu.VMEM((m, tokens, cols), bf16),
            pltpu.VMEM((m, tokens, cols), bf16),
            pltpu.VMEM((m, rank, rank), f32),
            pltpu.VMEM((n, rows, cols), bf16),
            pltpu.VMEM((n, rows, cols), bf16),
            pltpu.VMEM((reach, channels), bf16),
            pltpu.VMEM((groups, reach + tokens, LANES), f32),
            pltpu.VMEM((groups, tokens, LANES), f32),
            pltpu.VMEM((groups * padded, LANES), f32),
            pltpu.VMEM((n, chunk, LANES), bf16),
            pltpu.VMEM((n, chunk, LANES), bf16),
            pltpu.VMEM((n, chunk, LANES), bf16),
            pltpu.VMEM((m, rows, cols), f32),
            dma((m,)),
            dma((m,)),
            dma((m,)),
            dma((m,)),
            dma((n,)),
            dma((n,)),
            dma,
            dma,
            dma((n,)),
            dma((n,)),
            dma((n,)),
            dma((n,)),
            dma((m,)),
            dma((m,)),
        ],
        compiler_params=pltpu.CompilerParams(collective_id=0, has_side_effects=True),
        name="reduce",
    )(x, v, g, c, f, m1, m2)

    steps = 4 if features % (4 * LANES) == 0 else 1
    block = features // steps
    whole = lambda a: pl.BlockSpec(a.shape, lambda i: (0, 0))
    wide = pl.BlockSpec((rows, block), lambda i: (0, i))
    return pl.pallas_call(
        update_kernel,
        grid=(steps,),
        out_shape=(
            jax.ShapeDtypeStruct(w.shape, f32),
            jax.ShapeDtypeStruct(w.shape, bf16),
            jax.ShapeDtypeStruct(w.shape, f32),
            jax.ShapeDtypeStruct(m1.shape, f32),
            jax.ShapeDtypeStruct(m1.shape, f32),
            jax.ShapeDtypeStruct(k.shape, f32),
            jax.ShapeDtypeStruct(k.shape, f32),
            jax.ShapeDtypeStruct(k.shape, f32),
        ),
        in_specs=[
            whole(dn),
            pl.BlockSpec((block, rank), lambda i: (i, 0)),
            wide,
            whole(proj),
            whole(m1),
            whole(m2),
            whole(kg),
            whole(k),
            whole(k1),
            whole(k2),
        ],
        out_specs=(wide, wide, wide, whole(m1), whole(m1), whole(k), whole(k), whole(k)),
        compiler_params=pltpu.CompilerParams(dimension_semantics=("arbitrary",)),
        name="update",
    )(dn, f, w, proj, m1, m2, kg, k, k1, k2)


def solution(mesh):
    both, rows, cols = P("fs", "tp"), P("fs", None), P(None, "tp")
    return jax.shard_map(
        functools.partial(body, mesh.shape["fs"], mesh.shape["tp"]),
        mesh=mesh,
        in_specs=(both, rows, both, both, P("tp", None), both, both, both, cols, cols, cols),
        out_specs=(both, both, both, both, both, cols, cols, cols),
        check_vma=False,
    )
```

```python
import functools

import jax
import jax.numpy as jnp
from jax import lax
from jax.experimental import pallas as pl
from jax.experimental.pallas import tpu as pltpu
from jax.sharding import PartitionSpec as P

MESH = pl.DeviceIdType.MESH
LANES = 128
f32 = jnp.float32
bf16 = jnp.bfloat16


def remote(src, dst, send, recv, axis, peer):
    return pltpu.make_async_remote_copy(
        src_ref=src,
        dst_ref=dst,
        send_sem=send,
        recv_sem=recv,
        device_id={axis: peer},
        device_id_type=MESH,
    )


def reduce_kernel(
    n,
    m,
    x_hbm,
    v_hbm,
    g_hbm,
    c_hbm,
    f_hbm,
    m1_hbm,
    m2_hbm,
    proj_ref,
    kg_ref,
    dn_ref,
    x_ref,
    v_ref,
    g_ref,
    c_ref,
    f_ref,
    m1_ref,
    m2_ref,
    load_s,
    low_out,
    low_in,
    gram,
    part,
    recv,
    halo,
    ext,
    cot,
    stage,
    tap_out,
    tap_in,
    tap_all,
    dirs,
    low_s,
    low_r,
    gram_s,
    gram_r,
    bulk_s,
    bulk_r,
    halo_s,
    halo_r,
    tap_s,
    tap_r,
    all_s,
    all_r,
    dir_s,
    dir_r,
):
    me = lax.axis_index("fs")
    my = lax.axis_index("tp")
    tokens = x_ref.shape[0]
    width = f_ref.shape[0] * m
    rows, cols = m1_ref.shape
    reach = halo.shape[0]
    groups = ext.shape[0]
    taps = kg_ref.shape[0]
    padded = stage.shape[0] // groups

    def peers(count, own, fn):
        def step(off, carry):
            fn(off, lax.rem(own + off, count))
            return carry

        lax.fori_loop(1, count, step, 0)

    def far_first(fn):
        half = n // 2
        side, place = me // half, lax.rem(me, half)

        def across(j, carry):
            fn(j, (1 - side) * half + lax.rem(place + j, half))
            return carry

        def along(j, carry):
            fn(half + j, side * half + lax.rem(place + j, half))
            return carry

        lax.fori_loop(0, half, across, 0)
        lax.fori_loop(1, half, along, 0)

    barrier = pltpu.get_barrier_semaphore()
    peers(n, me, lambda off, p: pl.semaphore_signal(barrier, inc=1, device_id={"fs": p}, device_id_type=MESH))
    peers(m, my, lambda off, p: pl.semaphore_signal(barrier, inc=1, device_id={"tp": p}, device_id_type=MESH))

    pairs = [(x_hbm, x_ref), (f_hbm, f_ref), (g_hbm, g_ref), (c_hbm, c_ref)]
    pairs += [(v_hbm, v_ref), (m1_hbm, m1_ref), (m2_hbm, m2_ref)]
    loads = [pltpu.make_async_copy(a, b, load_s.at[i]) for i, (a, b) in enumerate(pairs)]
    for load in loads:
        load.start()
    loads[0].wait()
    loads[1].wait()

    low = jnp.dot(x_ref[...], f_ref[...], preferred_element_type=f32).astype(bf16)
    for j in range(m):
        low_out[j] = low[:, j * cols : (j + 1) * cols]

    loads[2].wait()
    loads[3].wait()
    for g in range(groups):
        lanes = slice(g * LANES, (g + 1) * LANES)
        ext[g, :reach] = jnp.zeros((reach, LANES), f32)
        ext[g, reach:] = g_ref[:, lanes].astype(f32)
        cot[g] = c_ref[:, lanes].astype(f32)

    def group_step(count, add):
        def step(g, carry):
            right = cot[g, :count, :]
            sums = []
            for k in range(taps):
                product = ext[g, pl.ds(reach - k, count), :] * right
                sums.append(jnp.sum(product, axis=0, keepdims=True))
            sums.append(jnp.zeros((padded - taps, LANES), f32))
            at = pl.ds(pl.multiple_of(g * padded, padded), padded)
            block = jnp.concatenate(sums, axis=0)
            stage[at, :] = stage[at, :] + block if add else block
            return carry

        lax.fori_loop(0, groups, step, 0)

    group_step(tokens, False)

    pl.semaphore_wait(barrier, n - 1 + m - 1)

    def low_copy(off, p):
        return remote(low_out.at[p], low_in.at[my], low_s.at[off], low_r.at[off], "tp", p)

    peers(m, my, lambda off, p: low_copy(off, p).start())
    low_in[my] = low_out[my]
    after = lax.rem(me + 1, n)
    halo_copy = remote(
        g_ref.at[pl.ds(tokens - reach, reach)], halo, halo_s, halo_r, "fs", after
    )
    halo_copy.start()

    halo_copy.wait()
    halo_f = jnp.where(me > 0, halo[...].astype(f32), 0.0)
    for g in range(groups):
        ext[g, :reach] = halo_f[:, g * LANES : (g + 1) * LANES]
        ext[g, reach:] = jnp.zeros((tokens, LANES), f32)
    group_step(reach, True)
    tap_out[...] = stage[...].reshape(tap_out.shape).astype(bf16)

    def tap_copy(off, p):
        return remote(tap_out.at[p], tap_in.at[me], tap_s.at[off], tap_r.at[off], "fs", p)

    peers(n, me, lambda off, p: tap_copy(off, p).start())
    tap_in[me] = tap_out[me]
    loads[4].wait()

    peers(m, my, lambda off, p: low_copy(off, p).wait())
    reduced = low_in[0].astype(f32)
    for j in range(1, m):
        reduced = reduced + low_in[j].astype(f32)
    reduced = reduced.astype(bf16)

    part[...] = (
        lax.dot_general(v_ref[...], reduced, (((0,), (0,)), ((), ())), preferred_element_type=f32)
        .astype(bf16)
        .reshape(n, rows, cols)
    )

    def bulk_copy(off, p):
        return remote(part.at[p], recv.at[me], bulk_s.at[off], bulk_r.at[off], "fs", p)

    far_first(lambda off, p: bulk_copy(off, p).start())
    recv[me] = part[me]

    gram[my] = lax.dot_general(
        f_ref[...], f_ref[...], (((0,), (0,)), ((), ())), preferred_element_type=f32
    )

    def gram_copy(off, p):
        return remote(gram.at[my], gram.at[my], gram_s.at[off], gram_r.at[off], "tp", p)

    peers(m, my, lambda off, p: gram_copy(off, p).start())

    peers(n, me, lambda off, p: tap_copy(off, p).wait())
    tap_all[me] = jnp.sum(tap_in[...].astype(f32), axis=0).astype(bf16)

    def all_copy(off, p):
        return remote(tap_all.at[me], tap_all.at[me], all_s.at[off], all_r.at[off], "fs", p)

    peers(n, me, lambda off, p: all_copy(off, p).start())

    loads[5].wait()
    loads[6].wait()
    far_first(lambda off, p: bulk_copy(off, p).wait())
    projected = recv[0].astype(f32)
    for j in range(1, n):
        projected = projected + recv[j].astype(f32)
    proj_ref[...] = projected
    first = 0.8 * m1_ref[...] + 0.2 * projected
    second = 0.9 * m2_ref[...] + 0.1 * projected * projected
    dirs[my] = first / jnp.sqrt(second)

    def dir_copy(off, p):
        return remote(dirs.at[my], dirs.at[my], dir_s.at[off], dir_r.at[off], "tp", p)

    peers(m, my, lambda off, p: dir_copy(off, p).start())

    peers(m, my, lambda off, p: gram_copy(off, p).wait())
    total = gram[0]
    for j in range(1, m):
        total = total + gram[j]
    peers(m, my, lambda off, p: dir_copy(off, p).wait())
    direction = jnp.concatenate([dirs[j] for j in range(m)], axis=1)
    turned = jnp.dot(direction, total, precision=lax.Precision.HIGHEST, preferred_element_type=f32)
    mean = jnp.sum(turned * direction, axis=1, keepdims=True) / width
    dn_ref[...] = (direction / jnp.sqrt(mean + 0.01)).astype(bf16)

    peers(n, me, lambda off, p: all_copy(off, p).wait())
    stage[...] = tap_all[...].astype(f32).reshape(stage.shape)
    for g in range(groups):
        kg_ref[:, g * LANES : (g + 1) * LANES] = stage[g * padded : g * padded + taps, :]


def update_kernel(steps, *refs):
    source, target, local, made = refs[:10], refs[10:18], refs[18:28], refs[28:36]
    small_s, f_s, w_s, out_s, wide_s = refs[36:]
    dn_ref, f_ref, w_ref, proj_ref, m1_ref, m2_ref, kg_ref, k_ref, k1_ref, k2_ref = local
    value_ref, copy_ref, step_ref, n1_ref, n2_ref, nk_ref, nk1_ref, nk2_ref = made
    block = f_ref.shape[0] // steps
    spans = [pl.ds(i * block, block) for i in range(steps)]
    copy = pltpu.make_async_copy
    small = {i: copy(source[i], local[i], small_s.at[i]) for i in (0, 3, 4, 5, 6, 7, 8, 9)}
    f_in = [copy(source[1].at[at], f_ref.at[at], f_s.at[i]) for i, at in enumerate(spans)]
    w_in = [copy(source[2].at[:, at], w_ref.at[:, at], w_s.at[i]) for i, at in enumerate(spans)]
    small[0].start()
    for i in range(steps):
        f_in[i].start()
        w_in[i].start()
    for i in range(3, 10):
        small[i].start()

    outs = []
    dims = (((1,), (1,)), ((), ()))
    small[0].wait()
    dn = dn_ref[...]
    for i, at in enumerate(spans):
        f_in[i].wait()
        step = lax.dot_general(dn, f_ref[at, :], dims, preferred_element_type=f32)
        w_in[i].wait()
        step_ref[:, at] = step
        value = w_ref[:, at] - 0.05 * step
        value_ref[:, at] = value
        copy_ref[:, at] = value.astype(bf16)
        for j in range(3):
            out = copy(made[j].at[:, at], target[j].at[:, at], wide_s.at[j, i])
            out.start()
            outs.append(out)

    for i in range(3, 10):
        small[i].wait()
    projected = proj_ref[...]
    n1_ref[...] = 0.8 * m1_ref[...] + 0.2 * projected
    n2_ref[...] = 0.9 * m2_ref[...] + 0.1 * projected * projected
    grad = kg_ref[...]
    first = 0.8 * k1_ref[...] + 0.2 * grad
    second = 0.9 * k2_ref[...] + 0.1 * grad * grad
    nk1_ref[...] = first
    nk2_ref[...] = second
    nk_ref[...] = k_ref[...] - 0.05 * first / jnp.sqrt(second)
    for j in range(3, 8):
        out = copy(made[j], target[j], out_s.at[j])
        out.start()
        outs.append(out)
    for out in outs:
        out.wait()


def body(n, m, x, v, g, c, f, w, m1, m2, k, k1, k2):
    tokens = x.shape[0]
    features, rank = f.shape
    rows, cols = m1.shape
    taps, channels = k.shape
    groups = channels // LANES
    reach = -(-(taps - 1) // 16) * 16
    padded = -(-taps // 8) * 8
    chunk = groups * padded // n
    vmem = pl.BlockSpec(memory_space=pltpu.VMEM)
    dma = pltpu.SemaphoreType.DMA
    proj, kg, dn = pl.pallas_call(
        functools.partial(reduce_kernel, n, m),
        out_shape=(
            jax.ShapeDtypeStruct((rows, cols), f32),
            jax.ShapeDtypeStruct((taps, channels), f32),
            jax.ShapeDtypeStruct((rows, rank), bf16),
        ),
        in_specs=[pl.BlockSpec(memory_space=pl.ANY)] * 7,
        out_specs=(vmem,) * 3,
        scratch_shapes=[
            *(pltpu.VMEM(a.shape, a.dtype) for a in (x, v, g, c, f, m1, m2)),
            dma((7,)),
            pltpu.VMEM((m, tokens, cols), bf16),
            pltpu.VMEM((m, tokens, cols), bf16),
            pltpu.VMEM((m, rank, rank), f32),
            pltpu.VMEM((n, rows, cols), bf16),
            pltpu.VMEM((n, rows, cols), bf16),
            pltpu.VMEM((reach, channels), bf16),
            pltpu.VMEM((groups, reach + tokens, LANES), f32),
            pltpu.VMEM((groups, tokens, LANES), f32),
            pltpu.VMEM((groups * padded, LANES), f32),
            pltpu.VMEM((n, chunk, LANES), bf16),
            pltpu.VMEM((n, chunk, LANES), bf16),
            pltpu.VMEM((n, chunk, LANES), bf16),
            pltpu.VMEM((m, rows, cols), f32),
            dma((m,)),
            dma((m,)),
            dma((m,)),
            dma((m,)),
            dma((n,)),
            dma((n,)),
            dma,
            dma,
            dma((n,)),
            dma((n,)),
            dma((n,)),
            dma((n,)),
            dma((m,)),
            dma((m,)),
        ],
        compiler_params=pltpu.CompilerParams(collective_id=0, has_side_effects=True),
        name="reduce",
    )(x, v, g, c, f, m1, m2)

    steps = 4 if features % (4 * LANES) == 0 else 1
    operands = (dn, f, w, proj, m1, m2, kg, k, k1, k2)
    results = (
        jax.ShapeDtypeStruct(w.shape, f32),
        jax.ShapeDtypeStruct(w.shape, bf16),
        jax.ShapeDtypeStruct(w.shape, f32),
        jax.ShapeDtypeStruct(m1.shape, f32),
        jax.ShapeDtypeStruct(m1.shape, f32),
        jax.ShapeDtypeStruct(k.shape, f32),
        jax.ShapeDtypeStruct(k.shape, f32),
        jax.ShapeDtypeStruct(k.shape, f32),
    )
    hbm = pl.BlockSpec(memory_space=pl.ANY)
    return pl.pallas_call(
        functools.partial(update_kernel, steps),
        out_shape=results,
        in_specs=[hbm] * 10,
        out_specs=(hbm,) * 8,
        scratch_shapes=[
            *(pltpu.VMEM(a.shape, a.dtype) for a in operands),
            *(pltpu.VMEM(a.shape, a.dtype) for a in results),
            dma((10,)),
            dma((steps,)),
            dma((steps,)),
            dma((8,)),
            dma((3, steps)),
        ],
        name="update",
    )(*operands)


def solution(mesh):
    both, rows, cols = P("fs", "tp"), P("fs", None), P(None, "tp")
    return jax.shard_map(
        functools.partial(body, mesh.shape["fs"], mesh.shape["tp"]),
        mesh=mesh,
        in_specs=(both, rows, both, both, P("tp", None), both, both, both, cols, cols, cols),
        out_specs=(both, both, both, both, both, cols, cols, cols),
        check_vma=False,
    )
```
